32 devices in a mesh: sp: 8 (over z, y), tp: 4 (over x, core).
Axes of the slice: x: 2, y: 2, z: 4, core: 2. Of those that a mesh axis runs over, the one named last changes fastest.
Arguments:
- latents: bfloat16 [5120, 2048], P('sp'), may hold values from -6 to 6
- cond: float32 [2048], replicated, may hold values from -6 to 6
- ctx_cond: float32 [2048], replicated, may hold values from -6 to 6
- context: bfloat16 [768, 2048], P('sp'), may hold values from -6 to 6
- norm_gain: float32 [2048], replicated, may hold values from 0.1 to 1.9
- shift_weight: bfloat16 [2048, 2048], P('tp'), may hold values from -0.125 to 0.125
- scale_weight: bfloat16 [2048, 2048], P('tp'), may hold values from -0.125 to 0.125
- gate_weight: bfloat16 [2048, 2048], P('tp'), may hold values from -0.125 to 0.125
- q_weight: bfloat16 [2048, 1024], P(None, 'tp'), may hold values from -0.125 to 0.125
- k_weight: bfloat16 [2048, 1024], P(None, 'tp'), may hold values from -0.125 to 0.125
- v_weight: bfloat16 [2048, 1024], P(None, 'tp'), may hold values from -0.125 to 0.125
- out_weight: bfloat16 [1024, 2048], replicated, may hold values from -1.5 to 1.5
- rel_bias: float32 [8, 15, 31], P('tp'), may hold values from 1.5 to 260
Outputs:
- result: bfloat16 [5120, 2048], P(('sp', 'tp'))
The draws below stay inside these ranges and needn't reach their ends.
All inputs are finite; a program needn't handle non-finite values.
Results may differ from the reference program's by a relative error of at most 0.0085.
Values may be sent and summed in bfloat16 or wider, within the bound.
No kernel may reach another device: no remote copies, remote signals or barrier semaphores. Data moves between devices by JAX's collectives and lax.ppermute only.
A program may use at most 64 MiB of HBM per device.

```python
import jax
import jax.numpy as jnp
from jax import lax

D = 2048
HEADS = 8
HEAD_DIM = 128
GRID_W = 64
WIN_ROWS = 8
WIN_COLS = 16
CTX = 768
ROWS = 80
TOKENS = 5120
NA_WIDTH = 1024


def draw_rel_bias(key, part):
    base_key = jax.random.fold_in(jax.random.fold_in(key, 4711), 0)
    table = jax.random.uniform(base_key, (HEADS, 2 * WIN_ROWS - 1, 2 * WIN_COLS - 1), jnp.float32, 1.5, 4.5)
    return table.astype(jnp.float32)


def block_scale(own_key, extent, cuts, low, top_value):
    def one(axis_at, parts):
        steps = jax.random.uniform(jax.random.fold_in(jax.random.fold_in(own_key, 6), axis_at), (parts,), jnp.float32, low / len(cuts), top_value / len(cuts))
        return jnp.repeat(jnp.exp(steps), extent[axis_at] // parts).reshape((-1,) + (1,) * (len(extent) - axis_at - 1))

    level = one(*cuts[0])
    for cut in cuts[1:]:
        level = level * one(*cut)
    return level


def noise(stream_key, shape, width, limit, cuts=(), kind=jnp.bfloat16):
    level = block_scale(stream_key, shape, cuts, -0.22, 0.18) if cuts else 1.0
    array = jax.random.normal(stream_key, shape, jnp.float32) * width * level
    return jnp.minimum(jnp.maximum(array, -limit), limit).astype(kind)


def setup_inputs(seed: int = 0) -> dict:
    key_list = jax.random.split(jax.random.key(seed), 14)
    return {
        "latents": noise(key_list[0], (TOKENS, D), 1.0, 6.0, ((0, 8),)),
        "cond": noise(key_list[1], (D,), 1.0, 6.0, (), jnp.float32),
        "ctx_cond": noise(key_list[2], (D,), 1.0, 6.0, (), jnp.float32),
        "context": noise(key_list[3], (CTX, D), 1.0, 6.0, ((0, 8),)),
        "norm_gain": jnp.clip(1.0 + 0.18 * jax.random.normal(key_list[4], (D,), jnp.float32), 0.1, 1.9),
        "shift_weight": noise(key_list[5], (D, D), D ** -0.5, 0.125, ((0, 4),)),
        "scale_weight": noise(key_list[6], (D, D), D ** -0.5, 0.125, ((0, 4),)),
        "gate_weight": noise(key_list[7], (D, D), D ** -0.5, 0.125, ((0, 4),)),
        "q_weight": noise(key_list[8], (D, NA_WIDTH), D ** -0.5, 0.125, ((1, 4),)),
        "k_weight": noise(key_list[9], (D, NA_WIDTH), D ** -0.5, 0.125, ((1, 4),)),
        "v_weight": noise(key_list[10], (D, NA_WIDTH), D ** -0.5, 0.125, ((1, 4),)),
        "out_weight": noise(key_list[11], (NA_WIDTH, D), (max(NA_WIDTH // 64, 1)) ** -0.5, 1.5),
        "rel_bias": draw_rel_bias(jax.random.fold_in(key_list[13], 71), 0),
    }


EPS = 1e-06
NEG_BIG = -1e+30

def modulated_norm(tok_rows, gain, shift_row, scale_row):
    rows_f = tok_rows.astype(jnp.float32)
    inverse = lax.rsqrt(lax.optimization_barrier(jnp.mean(rows_f * rows_f, axis=-1, keepdims=True)) + EPS)
    return (rows_f * inverse * gain * (1.0 + scale_row) + shift_row).astype(jnp.bfloat16)

def column_mask():
    columns = jnp.arange(GRID_W, dtype=jnp.int32)
    first_col = jnp.clip(columns - WIN_COLS // 2, 0, GRID_W - WIN_COLS)
    inside = (columns[None, :] >= first_col[:, None]) & (columns[None, :] < first_col[:, None] + WIN_COLS)
    return jnp.tile(inside, (1, WIN_ROWS))

def grid_bias(bias_table, row_diff):
    row_hot = (row_diff[:, :, None] == jnp.arange(2 * WIN_ROWS - 1, dtype=jnp.int32)[None, None, :]).astype(jnp.float32)
    columns = jnp.arange(GRID_W, dtype=jnp.int32)
    col_diff = jnp.clip(columns[None, :] - columns[:, None], -(WIN_COLS - 1), WIN_COLS - 1) + WIN_COLS - 1
    col_hot = (col_diff[:, :, None] == jnp.arange(2 * WIN_COLS - 1, dtype=jnp.int32)[None, None, :]).astype(jnp.float32)
    middle = jnp.einsum('rai,hij->hraj', row_hot, bias_table.astype(jnp.float32), precision=lax.Precision.HIGHEST)
    spread = jnp.einsum('hraj,qbj->hrqab', middle, col_hot, precision=lax.Precision.HIGHEST)
    return spread.reshape(bias_table.shape[0], row_diff.shape[0], GRID_W, WIN_ROWS * GRID_W)

def attend(query, key_win, val_win, ctx_keys, ctx_vals, bias, inside):
    factor = HEAD_DIM ** (-0.5)
    near_scores = jnp.einsum('rqhd,rkhd->hrqk', query.astype(jnp.float32), key_win.astype(jnp.float32)) * factor + bias
    near_scores = jnp.where(inside, near_scores, NEG_BIG)
    far_scores = jnp.einsum('rqhd,lhd->hrql', query.astype(jnp.float32), ctx_keys.astype(jnp.float32)) * factor
    row_peak = jnp.maximum(lax.optimization_barrier(jnp.max(near_scores, axis=-1, keepdims=True)), lax.optimization_barrier(jnp.max(far_scores, axis=-1, keepdims=True)))
    near_exp = jnp.exp(near_scores - row_peak)
    far_exp = jnp.exp(far_scores - row_peak)
    denominator = lax.optimization_barrier(jnp.sum(near_exp, axis=-1, keepdims=True)) + lax.optimization_barrier(jnp.sum(far_exp, axis=-1, keepdims=True))
    near_w = (near_exp / denominator).astype(jnp.bfloat16)
    far_w = (far_exp / denominator).astype(jnp.bfloat16)
    mixed = jnp.einsum('hrqk,rkhd->rqhd', near_w.astype(jnp.float32), val_win.astype(jnp.float32)) + jnp.einsum('hrql,lhd->rqhd', far_w.astype(jnp.float32), ctx_vals.astype(jnp.float32))
    return mixed.astype(jnp.bfloat16)

def reference(latents, cond, ctx_cond, context, norm_gain, shift_weight, scale_weight, gate_weight, q_weight, k_weight, v_weight, out_weight, rel_bias):
    conds = jnp.stack([cond, ctx_cond])
    active = jax.nn.silu(conds).astype(jnp.bfloat16)
    shifts = jnp.dot(active, shift_weight, preferred_element_type=jnp.float32)
    scales = jnp.dot(active, scale_weight, preferred_element_type=jnp.float32)
    gates = jnp.dot(active[:1], gate_weight, preferred_element_type=jnp.float32)
    h_lat = modulated_norm(latents, norm_gain, shifts[0], scales[0])
    h_ctx = modulated_norm(context, norm_gain, shifts[1], scales[1])
    query = jnp.dot(h_lat, q_weight, preferred_element_type=jnp.float32).astype(jnp.bfloat16)
    keys = jnp.dot(h_lat, k_weight, preferred_element_type=jnp.float32).astype(jnp.bfloat16)
    values = jnp.dot(h_lat, v_weight, preferred_element_type=jnp.float32).astype(jnp.bfloat16)
    ctx_keys = jnp.dot(h_ctx, k_weight, preferred_element_type=jnp.float32).astype(jnp.bfloat16)
    ctx_vals = jnp.dot(h_ctx, v_weight, preferred_element_type=jnp.float32).astype(jnp.bfloat16)
    grid_rows = jnp.arange(ROWS, dtype=jnp.int32)
    first_row = jnp.clip(grid_rows - WIN_ROWS // 2, 0, ROWS - WIN_ROWS)
    offsets = jnp.arange(WIN_ROWS, dtype=jnp.int32)
    row_index = first_row[:, None] + offsets[None, :]
    row_diff = row_index - grid_rows[:, None] + WIN_ROWS - 1
    inside = column_mask()
    query_grid = query.reshape(ROWS, GRID_W, HEADS, HEAD_DIM)
    key_grid = keys.reshape(ROWS, GRID_W, HEADS, HEAD_DIM)
    val_grid = values.reshape(ROWS, GRID_W, HEADS, HEAD_DIM)
    ctx_key3 = ctx_keys.reshape(CTX, HEADS, HEAD_DIM)
    ctx_val3 = ctx_vals.reshape(CTX, HEADS, HEAD_DIM)

    def one_head(head_id):
        query_head = lax.dynamic_slice_in_dim(query_grid, head_id, 1, 2)
        key_head = lax.dynamic_slice_in_dim(key_grid, head_id, 1, 2)[row_index]
        val_head = lax.dynamic_slice_in_dim(val_grid, head_id, 1, 2)[row_index]
        key_head = key_head.reshape(ROWS, WIN_ROWS * GRID_W, 1, HEAD_DIM)
        val_head = val_head.reshape(ROWS, WIN_ROWS * GRID_W, 1, HEAD_DIM)
        ctx_key_head = lax.dynamic_slice_in_dim(ctx_key3, head_id, 1, 1)
        ctx_val_head = lax.dynamic_slice_in_dim(ctx_val3, head_id, 1, 1)
        bias = grid_bias(lax.dynamic_slice_in_dim(rel_bias, head_id, 1, 0), row_diff)
        return attend(query_head, key_head, val_head, ctx_key_head, ctx_val_head, bias, inside)
    head_outs = lax.map(one_head, jnp.arange(HEADS, dtype=jnp.int32))
    attn = jnp.transpose(head_outs[:, :, :, 0], (1, 2, 0, 3)).reshape(TOKENS, NA_WIDTH)
    mixed = jnp.dot(attn, out_weight, preferred_element_type=jnp.float32)
    return (latents.astype(jnp.float32) + gates[0] * mixed).astype(jnp.bfloat16)
```

```python
import functools

import jax
import jax.numpy as jnp
from jax import lax
from jax.experimental import pallas as pl
from jax.experimental.pallas import tpu as pltpu
from jax.sharding import PartitionSpec as P

HEAD_DIM = 128
GRID_W = 64
WIN_ROWS = 8
WIN_COLS = 16
HALF = WIN_ROWS // 2
EPS = 1e-06
NEG_BIG = -1e30


def shift_by(x, axis, k):
    n = lax.axis_size(axis)
    return lax.ppermute(x, axis, [(i, (i + k) % n) for i in range(n)])


def modulated_norm(tok_rows, gain, shift_row, scale_row):
    rows_f = tok_rows.astype(jnp.float32)
    inverse = lax.rsqrt(jnp.mean(rows_f * rows_f, axis=-1, keepdims=True) + EPS)
    return (rows_f * inverse * (gain * (1.0 + scale_row)) + shift_row).astype(jnp.bfloat16)


def bias_body(table_ref, out_ref):
    lane = lax.broadcasted_iota(jnp.int32, (GRID_W, 2 * GRID_W), 1)
    col = lane % GRID_W
    own = lax.broadcasted_iota(jnp.int32, (GRID_W, 2 * GRID_W), 0)
    first = jnp.clip(own - WIN_COLS // 2, 0, GRID_W - WIN_COLS)
    inside = (col >= first) & (col < first + WIN_COLS)
    low = lane < GRID_W
    for d in range(2 * WIN_ROWS - 2):
        left = jnp.broadcast_to(table_ref[0, d : d + 1, :], (GRID_W, 2 * GRID_W))
        right = jnp.broadcast_to(table_ref[0, d + 1 : d + 2, :], (GRID_W, 2 * GRID_W))
        left = pltpu.roll(left, 2 * GRID_W - (WIN_COLS - 1), 1, stride=1, stride_axis=0)
        right = pltpu.roll(right, GRID_W - (WIN_COLS - 1), 1, stride=1, stride_axis=0)
        out_ref[0, d] = jnp.where(inside, jnp.where(low, left, right), NEG_BIG)


def bias_tiles(rel_bias):
    heads = rel_bias.shape[0]
    table = jnp.pad(rel_bias, ((0, 0), (0, 1), (0, 2 * GRID_W - rel_bias.shape[2])))
    return pl.pallas_call(
        bias_body,
        grid=(heads,),
        in_specs=[pl.BlockSpec((1,) + table.shape[1:], lambda h: (h, 0, 0))],
        out_specs=pl.BlockSpec((1, 2 * WIN_ROWS - 2, GRID_W, 2 * GRID_W), lambda h: (h, 0, 0, 0)),
        out_shape=jax.ShapeDtypeStruct((heads, 2 * WIN_ROWS - 2, GRID_W, 2 * GRID_W), jnp.float32),
        name="bias_tiles",
    )(table)


def attend_body(rows_here, group, place_ref, q_ref, k_ref, v_ref, ck_ref, cv_ref, bias_ref, out_ref):
    factor = HEAD_DIM ** (-0.5)
    base, total = place_ref[0], place_ref[1]
    contract_last = (((1,), (1,)), ((), ()))
    plain = (((1,), (0,)), ((), ()))
    for r0 in range(0, rows_here, group):
        q = q_ref[r0 * GRID_W : (r0 + group) * GRID_W, :]
        far = lax.dot_general(q, ck_ref[...], contract_last, preferred_element_type=jnp.float32) * factor
        near, starts = [], []
        for g in range(group):
            row = base + r0 + g
            first = jnp.clip(row - HALF, 0, total - WIN_ROWS)
            start = pl.multiple_of((first - base + HALF) * GRID_W, GRID_W)
            delta = first - row + WIN_ROWS - 1
            keys = k_ref[pl.ds(start, WIN_ROWS * GRID_W), :]
            part = lax.dot_general(q[g * GRID_W : (g + 1) * GRID_W], keys, contract_last, preferred_element_type=jnp.float32)
            bias = jnp.concatenate([bias_ref[0, delta + 2 * t] for t in range(WIN_ROWS // 2)], axis=1)
            near.append(part * factor + bias)
            starts.append(start)
        near = jnp.concatenate(near, axis=0)
        peak = jnp.maximum(jnp.max(near, axis=1, keepdims=True), jnp.max(far, axis=1, keepdims=True))
        near = jnp.exp(near - peak)
        far = jnp.exp(far - peak)
        inverse = 1.0 / (jnp.sum(near, axis=1, keepdims=True) + jnp.sum(far, axis=1, keepdims=True))
        near = near.astype(jnp.bfloat16)
        mixed = lax.dot_general(far.astype(jnp.bfloat16), cv_ref[...], plain, preferred_element_type=jnp.float32)
        local = [
            lax.dot_general(
                near[g * GRID_W : (g + 1) * GRID_W], v_ref[pl.ds(starts[g], WIN_ROWS * GRID_W), :],
                plain, preferred_element_type=jnp.float32)
            for g in range(group)
        ]
        mixed = (mixed + jnp.concatenate(local, axis=0)) * inverse
        out_ref[r0 * GRID_W : (r0 + group) * GRID_W, :] = mixed.astype(jnp.bfloat16)


def attend(place, query, padded, ctx, bias):
    tokens, width = query.shape
    heads = width // HEAD_DIM
    rows_here = tokens // GRID_W
    group = 2 if rows_here % 2 == 0 else 1
    pad_n, ctx_n = padded.shape[0], ctx.shape[0]
    return pl.pallas_call(
        functools.partial(attend_body, rows_here, group),
        grid=(heads,),
        in_specs=[
            pl.BlockSpec(memory_space=pltpu.SMEM),
            pl.BlockSpec((tokens, HEAD_DIM), lambda h: (0, h)),
            pl.BlockSpec((pad_n, HEAD_DIM), lambda h: (0, h)),
            pl.BlockSpec((pad_n, HEAD_DIM), lambda h: (0, h + heads)),
            pl.BlockSpec((ctx_n, HEAD_DIM), lambda h: (0, h)),
            pl.BlockSpec((ctx_n, HEAD_DIM), lambda h: (0, h + heads)),
            pl.BlockSpec((1,) + bias.shape[1:], lambda h: (h, 0, 0, 0)),
        ],
        out_specs=pl.BlockSpec((tokens, HEAD_DIM), lambda h: (0, h)),
        out_shape=jax.ShapeDtypeStruct((tokens, width), jnp.bfloat16),
        name="attend",
    )(place, query, padded, padded, ctx, ctx, bias)


def out_body(count, tp_ref, *refs):
    pieces, (w_ref, gate_ref, lat_ref, out_ref) = refs[:count], refs[count:]
    me = tp_ref[0]
    depth = pieces[0].shape[1]
    mixed = None
    for k, piece in enumerate(pieces):
        at = lax.rem(me + (count - k), count)
        rows = w_ref[pl.ds(pl.multiple_of(at * depth, depth), depth), :]
        part = jnp.dot(piece[...], rows, preferred_element_type=jnp.float32)
        mixed = part if mixed is None else mixed + part
    out_ref[...] = (lat_ref[...].astype(jnp.float32) + gate_ref[...] * mixed).astype(jnp.bfloat16)


def project_out(me, pieces, out_weight, gates, latents):
    count = len(pieces)
    rows, depth = pieces[0].shape
    width = out_weight.shape[1]
    block = min(512, width)
    whole = lambda shape: pl.BlockSpec(shape, lambda n, s: (0, 0))
    return pl.pallas_call(
        functools.partial(out_body, count),
        grid_spec=pltpu.PrefetchScalarGridSpec(
            num_scalar_prefetch=1,
            grid=(width // block,),
            in_specs=[whole((rows, depth))] * count + [
                pl.BlockSpec((out_weight.shape[0], block), lambda n, s: (0, n)),
                pl.BlockSpec((1, block), lambda n, s: (0, n)),
                pl.BlockSpec((rows, block), lambda n, s: (s[0], n)),
            ],
            out_specs=pl.BlockSpec((rows, block), lambda n, s: (0, n)),
        ),
        out_shape=jax.ShapeDtypeStruct((rows, width), jnp.bfloat16),
        name="project_out",
    )(me, *pieces, out_weight, gates, latents)


def shards(
    latents, cond, ctx_cond, context, norm_gain, shift_weight, scale_weight, gate_weight,
    q_weight, k_weight, v_weight, out_weight, rel_bias,
):
    tp = lax.axis_size("tp")
    sp = lax.axis_size("sp")
    tp_at = lax.axis_index("tp")
    sp_at = lax.axis_index("sp")
    tp_rows = shift_weight.shape[0]
    conds = jnp.stack([cond, ctx_cond])
    active = jax.nn.silu(
        lax.dynamic_slice_in_dim(conds, tp_at * tp_rows, tp_rows, 1)
    ).astype(jnp.bfloat16)
    shifts = jnp.dot(active, shift_weight, preferred_element_type=jnp.float32)
    scales = jnp.dot(active, scale_weight, preferred_element_type=jnp.float32)
    gates = jnp.dot(active[:1], gate_weight, preferred_element_type=jnp.float32)
    mod = jnp.concatenate([shifts, scales, gates], axis=0)
    mod = functools.reduce(jnp.add, [shift_by(mod, "tp", k) for k in range(1, tp)], mod)
    shifts, scales, gates = mod[0:2], mod[2:4], mod[4:5]

    h_ctx = modulated_norm(context, norm_gain, shifts[1], scales[1])
    ctx_kv = jnp.concatenate(
        [jnp.dot(h_ctx, w, preferred_element_type=jnp.float32).astype(jnp.bfloat16) for w in (k_weight, v_weight)],
        axis=1,
    )
    ctx = jnp.concatenate([ctx_kv] + [shift_by(ctx_kv, "sp", k) for k in range(1, sp)], axis=0)

    h_lat = modulated_norm(latents, norm_gain, shifts[0], scales[0])
    kv = jnp.concatenate(
        [jnp.dot(h_lat, w, preferred_element_type=jnp.float32).astype(jnp.bfloat16) for w in (k_weight, v_weight)],
        axis=1,
    )
    halo = HALF * GRID_W
    up = [(i, i + 1) for i in range(sp - 1)]
    down = [(i + 1, i) for i in range(sp - 1)]
    before = lax.ppermute(kv[-halo:], "sp", up)
    after = lax.ppermute(kv[:halo], "sp", down)
    query = jnp.dot(h_lat, q_weight, preferred_element_type=jnp.float32).astype(jnp.bfloat16)
    padded = jnp.concatenate([before, kv, after], axis=0)

    rows_here = latents.shape[0] // GRID_W
    place = jnp.stack([sp_at * rows_here, jnp.int32(sp * rows_here)]).astype(jnp.int32)
    attn = attend(place, query, padded, ctx, bias_tiles(rel_bias))

    own = latents.shape[0] // tp
    pieces = []
    for k in range(tp):
        part = lax.dynamic_slice_in_dim(attn, lax.rem(tp_at + k, tp) * own, own, 0)
        pieces.append(shift_by(part, "tp", k) if k else part)
    return project_out(tp_at.reshape(1).astype(jnp.int32), pieces, out_weight, gates, latents)


def solution(mesh):
    in_specs = (
        P("sp", None), P(), P(), P("sp", None), P(), P("tp", None), P("tp", None), P("tp", None),
        P(None, "tp"), P(None, "tp"), P(None, "tp"), P(), P("tp", None, None),
    )
    out_specs = P(("sp", "tp"), None)
    return jax.shard_map(shards, mesh=mesh, in_specs=in_specs, out_specs=out_specs, check_vma=False)
```

```python
import functools

import jax
import jax.numpy as jnp
from jax import lax
from jax.experimental import pallas as pl
from jax.experimental.pallas import tpu as pltpu
from jax.sharding import PartitionSpec as P

HEAD_DIM = 128
GRID_W = 64
WIN_ROWS = 8
WIN_COLS = 16
HALF = WIN_ROWS // 2
EPS = 1e-06
NEG_BIG = -1e30


def shift_by(x, axis, k):
    n = lax.axis_size(axis)
    return lax.ppermute(x, axis, [(i, (i + k) % n) for i in range(n)])


def modulated_norm(tok_rows, gain, shift_row, scale_row):
    rows_f = tok_rows.astype(jnp.float32)
    inverse = lax.rsqrt(jnp.mean(rows_f * rows_f, axis=-1, keepdims=True) + EPS)
    return (rows_f * inverse * (gain * (1.0 + scale_row)) + shift_row).astype(jnp.bfloat16)


def bias_body(table_ref, out_ref):
    lane = lax.broadcasted_iota(jnp.int32, (GRID_W, 2 * GRID_W), 1)
    col = lane % GRID_W
    own = lax.broadcasted_iota(jnp.int32, (GRID_W, 2 * GRID_W), 0)
    first = jnp.clip(own - WIN_COLS // 2, 0, GRID_W - WIN_COLS)
    inside = (col >= first) & (col < first + WIN_COLS)
    low = lane < GRID_W
    for d in range(2 * WIN_ROWS - 2):
        left = jnp.broadcast_to(table_ref[0, d : d + 1, :], (GRID_W, 2 * GRID_W))
        right = jnp.broadcast_to(table_ref[0, d + 1 : d + 2, :], (GRID_W, 2 * GRID_W))
        left = pltpu.roll(left, 2 * GRID_W - (WIN_COLS - 1), 1, stride=1, stride_axis=0)
        right = pltpu.roll(right, GRID_W - (WIN_COLS - 1), 1, stride=1, stride_axis=0)
        out_ref[0, d] = jnp.where(inside, jnp.where(low, left, right), NEG_BIG)


def bias_tiles(rel_bias):
    heads = rel_bias.shape[0]
    table = jnp.pad(rel_bias, ((0, 0), (0, 1), (0, 2 * GRID_W - rel_bias.shape[2])))
    return pl.pallas_call(
        bias_body,
        grid=(heads,),
        in_specs=[pl.BlockSpec((1,) + table.shape[1:], lambda h: (h, 0, 0))],
        out_specs=pl.BlockSpec((1, 2 * WIN_ROWS - 2, GRID_W, 2 * GRID_W), lambda h: (h, 0, 0, 0)),
        out_shape=jax.ShapeDtypeStruct((heads, 2 * WIN_ROWS - 2, GRID_W, 2 * GRID_W), jnp.float32),
        name="bias_tiles",
    )(table)


def attend_body(group, halos, place_ref, q_ref, k_ref, v_ref, up_ref, down_ref, bias_ref, *refs):
    chunks, outs, (kv_ref, ctx_ref, attn_ref) = refs[: halos[2]], refs[halos[2] : -3], refs[-3:]
    factor = HEAD_DIM ** (-0.5)
    base, total, me = place_ref[0], place_ref[1], place_ref[2]
    tokens, width = q_ref.shape
    above, below = halos[0], halos[1]
    kv_ref[0:above, :] = up_ref[...]
    kv_ref[above : above + tokens, 0:width] = k_ref[...]
    kv_ref[above : above + tokens, width:] = v_ref[...]
    kv_ref[above + tokens : above + tokens + below, :] = down_ref[...]
    size = chunks[0].shape[0]
    for c, chunk in enumerate(chunks):
        ctx_ref[c * size : (c + 1) * size, :] = chunk[...]
    contract_last = (((1,), (1,)), ((), ()))
    plain = (((1,), (0,)), ((), ()))
    span = WIN_ROWS * GRID_W
    for h in range(width // HEAD_DIM):
        ks = slice(h * HEAD_DIM, (h + 1) * HEAD_DIM)
        vs = slice(width + h * HEAD_DIM, width + (h + 1) * HEAD_DIM)
        for r0 in range(0, tokens // GRID_W, group):
            at = slice(r0 * GRID_W, (r0 + group) * GRID_W)
            q = q_ref[at, ks]
            far = lax.dot_general(q, ctx_ref[:, ks], contract_last, preferred_element_type=jnp.float32) * factor
            near, starts = [], []
            for g in range(group):
                row = base + r0 + g
                first = jnp.clip(row - HALF, 0, total - WIN_ROWS)
                start = pl.multiple_of((first - base + HALF) * GRID_W, GRID_W)
                delta = first - row + WIN_ROWS - 1
                keys = kv_ref[pl.ds(start, span), ks]
                part = lax.dot_general(q[g * GRID_W : (g + 1) * GRID_W], keys, contract_last, preferred_element_type=jnp.float32)
                bias = jnp.concatenate([bias_ref[h, delta + 2 * t] for t in range(WIN_ROWS // 2)], axis=1)
                near.append(part * factor + bias)
                starts.append(start)
            near = jnp.concatenate(near, axis=0)
            peak = jnp.maximum(jnp.max(near, axis=1, keepdims=True), jnp.max(far, axis=1, keepdims=True))
            near = jnp.exp(near - peak)
            far = jnp.exp(far - peak)
            inverse = 1.0 / (jnp.sum(near, axis=1, keepdims=True) + jnp.sum(far, axis=1, keepdims=True))
            near = near.astype(jnp.bfloat16)
            mixed = lax.dot_general(far.astype(jnp.bfloat16), ctx_ref[:, vs], plain, preferred_element_type=jnp.float32)
            local = [
                lax.dot_general(
                    near[g * GRID_W : (g + 1) * GRID_W], kv_ref[pl.ds(starts[g], span), vs],
                    plain, preferred_element_type=jnp.float32)
                for g in range(group)
            ]
            mixed = (mixed + jnp.concatenate(local, axis=0)) * inverse
            attn_ref[at, ks] = mixed.astype(jnp.bfloat16)
    count = len(outs)
    own = tokens // count
    for k, out in enumerate(outs):
        block = lax.rem(me + k, count)
        out[...] = attn_ref[pl.ds(pl.multiple_of(block * own, own), own), :]


def attend(place, query, keys, values, before, after, bias, chunks, count):
    tokens, width = query.shape
    group = 2 if (tokens // GRID_W) % 2 == 0 else 1
    above, below = before.shape[0], after.shape[0]
    ctx_n = len(chunks) * chunks[0].shape[0]
    vmem = pl.BlockSpec(memory_space=pltpu.VMEM)
    return pl.pallas_call(
        functools.partial(attend_body, group, (above, below, len(chunks))),
        in_specs=[pl.BlockSpec(memory_space=pltpu.SMEM)] + [vmem] * (6 + len(chunks)),
        out_specs=[vmem] * count,
        out_shape=[jax.ShapeDtypeStruct((tokens // count, width), jnp.bfloat16)] * count,
        scratch_shapes=[
            pltpu.VMEM((above + tokens + below, 2 * width), jnp.bfloat16),
            pltpu.VMEM((ctx_n, 2 * width), jnp.bfloat16),
            pltpu.VMEM((tokens, width), jnp.bfloat16),
        ],
        compiler_params=pltpu.CompilerParams(vmem_limit_bytes=24 * 2**20),
        name="attend",
    )(place, query, keys, values, before, after, bias, *chunks)


def out_body(count, tp_ref, *refs):
    pieces, (w_ref, gate_ref, lat_ref, out_ref) = refs[:count], refs[count:]
    me = tp_ref[0]
    depth = pieces[0].shape[1]
    block = min(512, w_ref.shape[1])
    for n in range(0, w_ref.shape[1], block):
        cols = slice(n, n + block)
        mixed = None
        for k, piece in enumerate(pieces):
            at = lax.rem(me + (count - k), count)
            rows = w_ref[pl.ds(pl.multiple_of(at * depth, depth), depth), cols]
            part = jnp.dot(piece[...], rows, preferred_element_type=jnp.float32)
            mixed = part if mixed is None else mixed + part
        out_ref[:, cols] = (lat_ref[:, cols].astype(jnp.float32) + gate_ref[:, cols] * mixed).astype(jnp.bfloat16)


def project_out(me, pieces, out_weight, gates, residual):
    vmem = pl.BlockSpec(memory_space=pltpu.VMEM)
    return pl.pallas_call(
        functools.partial(out_body, len(pieces)),
        in_specs=[pl.BlockSpec(memory_space=pltpu.SMEM)] + [vmem] * (len(pieces) + 3),
        out_specs=vmem,
        out_shape=jax.ShapeDtypeStruct(residual.shape, jnp.bfloat16),
        compiler_params=pltpu.CompilerParams(vmem_limit_bytes=24 * 2**20),
        name="project_out",
    )(me, *pieces, out_weight, gates, residual)


def shards(
    latents, cond, ctx_cond, context, norm_gain, shift_weight, scale_weight, gate_weight,
    q_weight, k_weight, v_weight, out_weight, rel_bias,
):
    tp = lax.axis_size("tp")
    sp = lax.axis_size("sp")
    tp_at = lax.axis_index("tp")
    sp_at = lax.axis_index("sp")
    tp_rows = shift_weight.shape[0]
    after_this = lambda x, y: lax.optimization_barrier((x, y))[0]
    group = 2 if sp % 2 == 0 else 1
    near_ctx = context
    if group == 2:
        other = lax.ppermute(context, "sp", [(i, i ^ 1) for i in range(sp)])
        near_ctx = jnp.concatenate([context, other], axis=0)

    conds = jnp.stack([cond, ctx_cond])
    active = jax.nn.silu(
        lax.dynamic_slice_in_dim(conds, tp_at * tp_rows, tp_rows, 1)
    ).astype(jnp.bfloat16)
    shifts = jnp.dot(active, shift_weight, preferred_element_type=jnp.float32)
    scales = jnp.dot(active, scale_weight, preferred_element_type=jnp.float32)
    mod = jnp.concatenate([shifts, scales], axis=0)
    mod = functools.reduce(jnp.add, [shift_by(mod, "tp", k) for k in range(1, tp)], mod)
    shifts, scales = mod[0:2], mod[2:4]

    h_ctx = modulated_norm(near_ctx, norm_gain, shifts[1], scales[1])
    ctx_kv = jnp.concatenate(
        [jnp.dot(h_ctx, w, preferred_element_type=jnp.float32).astype(jnp.bfloat16) for w in (k_weight, v_weight)],
        axis=1,
    )
    chunks = [ctx_kv] + [shift_by(ctx_kv, "sp", k) for k in range(group, sp, group)]

    lat_shift, lat_scale = after_this((shifts[0], scales[0]), ctx_kv)
    h_lat = modulated_norm(latents, norm_gain, lat_shift, lat_scale)
    keys = jnp.dot(h_lat, k_weight, preferred_element_type=jnp.float32).astype(jnp.bfloat16)
    values = jnp.dot(h_lat, v_weight, preferred_element_type=jnp.float32).astype(jnp.bfloat16)
    above, below = HALF * GRID_W, (WIN_ROWS - HALF - 1) * GRID_W
    up = [(i, i + 1) for i in range(sp - 1)]
    down = [(i + 1, i) for i in range(sp - 1)]
    last = jnp.concatenate([keys[-above:], values[-above:]], axis=1)
    initial = jnp.concatenate([keys[:below], values[:below]], axis=1)
    before = lax.ppermute(last, "sp", up)
    after = lax.ppermute(initial, "sp", down)
    late_h, late_table, late_active = after_this((h_lat, rel_bias, active[:1]), (last, initial))
    query = jnp.dot(late_h, q_weight, preferred_element_type=jnp.float32).astype(jnp.bfloat16)
    gates = jnp.dot(late_active, gate_weight, preferred_element_type=jnp.float32)
    gates = functools.reduce(jnp.add, [shift_by(gates, "tp", k) for k in range(1, tp)], gates)

    rows_here = latents.shape[0] // GRID_W
    place = jnp.stack([sp_at * rows_here, jnp.int32(sp * rows_here), tp_at]).astype(jnp.int32)
    attn = attend(place, query, keys, values, before, after, bias_tiles(late_table), chunks, tp)
    pieces = [shift_by(part, "tp", k) if k else part for k, part in enumerate(attn)]
    own = latents.shape[0] // tp
    residual = lax.dynamic_slice_in_dim(latents, tp_at * own, own, 0)
    return project_out(tp_at.reshape(1).astype(jnp.int32), pieces, out_weight, gates, residual)


def solution(mesh):
    in_specs = (
        P("sp", None), P(), P(), P("sp", None), P(), P("tp", None), P("tp", None), P("tp", None),
        P(None, "tp"), P(None, "tp"), P(None, "tp"), P(), P("tp", None, None),
    )
    out_specs = P(("sp", "tp"), None)
    return jax.shard_map(shards, mesh=mesh, in_specs=in_specs, out_specs=out_specs, check_vma=False)
```

```python
import functools

import jax
import jax.numpy as jnp
from jax import lax
from jax.experimental import pallas as pl
from jax.experimental.pallas import tpu as pltpu
from jax.sharding import PartitionSpec as P

HEAD_DIM = 128
GRID_W = 64
WIN_ROWS = 8
WIN_COLS = 16
HALF = WIN_ROWS // 2
EPS = 1e-06
NEG_BIG = -1e30


def shift_by(x, axis, k):
    n = lax.axis_size(axis)
    return lax.ppermute(x, axis, [(i, (i + k) % n) for i in range(n)])


def modulated_norm(tok_rows, gain, shift_row, scale_row):
    rows_f = tok_rows.astype(jnp.float32)
    inverse = lax.rsqrt(jnp.mean(rows_f * rows_f, axis=-1, keepdims=True) + EPS)
    return (rows_f * inverse * (gain * (1.0 + scale_row)) + shift_row).astype(jnp.bfloat16)


def bias_body(table_ref, out_ref):
    lane = lax.broadcasted_iota(jnp.int32, (GRID_W, 2 * GRID_W), 1)
    col = lane % GRID_W
    own = lax.broadcasted_iota(jnp.int32, (GRID_W, 2 * GRID_W), 0)
    first = jnp.clip(own - WIN_COLS // 2, 0, GRID_W - WIN_COLS)
    inside = (col >= first) & (col < first + WIN_COLS)
    low = lane < GRID_W
    tiles = [(h, d) for h in range(table_ref.shape[0]) for d in range(2 * WIN_ROWS - 2)]
    for h, d in tiles:
        left = jnp.broadcast_to(table_ref[h, d : d + 1, :], (GRID_W, 2 * GRID_W))
        right = jnp.broadcast_to(table_ref[h, d + 1 : d + 2, :], (GRID_W, 2 * GRID_W))
        left = pltpu.roll(left, 2 * GRID_W - (WIN_COLS - 1), 1, stride=1, stride_axis=0)
        right = pltpu.roll(right, GRID_W - (WIN_COLS - 1), 1, stride=1, stride_axis=0)
        out_ref[h, d] = jnp.where(inside, jnp.where(low, left, right), NEG_BIG)


def bias_tiles(rel_bias):
    heads = rel_bias.shape[0]
    table = jnp.pad(rel_bias, ((0, 0), (0, 1), (0, 2 * GRID_W - rel_bias.shape[2])))
    return pl.pallas_call(
        bias_body,
        in_specs=[pl.BlockSpec(memory_space=pltpu.VMEM)],
        out_specs=pl.BlockSpec(memory_space=pltpu.VMEM),
        out_shape=jax.ShapeDtypeStruct((heads, 2 * WIN_ROWS - 2, GRID_W, 2 * GRID_W), jnp.float32),
        compiler_params=pltpu.CompilerParams(vmem_limit_bytes=8 * 2**20),
        name="bias_tiles",
    )(table)


def attend_body(group, halos, place_ref, q_ref, k_ref, v_ref, up_ref, down_ref, bias_ref, w_ref, *refs):
    chunks, outs, w_out = refs[: halos[2]], refs[halos[2] : -5], refs[-5]
    kv_ref, ctx_ref, attn_ref, sem = refs[-4:]
    fetch = pltpu.make_async_copy(w_ref, w_out, sem)
    fetch.start()
    factor = HEAD_DIM ** (-0.5)
    base, total, me = place_ref[0], place_ref[1], place_ref[2]
    tokens, width = q_ref.shape
    above, below = halos[0], halos[1]
    kv_ref[0:above, :] = up_ref[...]
    kv_ref[above : above + tokens, 0:width] = k_ref[...]
    kv_ref[above : above + tokens, width:] = v_ref[...]
    kv_ref[above + tokens : above + tokens + below, :] = down_ref[...]
    size = chunks[0].shape[0]
    for c, chunk in enumerate(chunks):
        ctx_ref[c * size : (c + 1) * size, :] = chunk[...]
    contract_last = (((1,), (1,)), ((), ()))
    plain = (((1,), (0,)), ((), ()))
    span = WIN_ROWS * GRID_W
    for h in range(width // HEAD_DIM):
        ks = slice(h * HEAD_DIM, (h + 1) * HEAD_DIM)
        vs = slice(width + h * HEAD_DIM, width + (h + 1) * HEAD_DIM)
        for r0 in range(0, tokens // GRID_W, group):
            at = slice(r0 * GRID_W, (r0 + group) * GRID_W)
            q = q_ref[at, ks]
            far = lax.dot_general(q, ctx_ref[:, ks], contract_last, preferred_element_type=jnp.float32) * factor
            near, starts = [], []
            for g in range(group):
                row = base + r0 + g
                first = jnp.clip(row - HALF, 0, total - WIN_ROWS)
                start = pl.multiple_of((first - base + HALF) * GRID_W, GRID_W)
                delta = first - row + WIN_ROWS - 1
                keys = kv_ref[pl.ds(start, span), ks]
                part = lax.dot_general(q[g * GRID_W : (g + 1) * GRID_W], keys, contract_last, preferred_element_type=jnp.float32)
                bias = jnp.concatenate([bias_ref[h, delta + 2 * t] for t in range(WIN_ROWS // 2)], axis=1)
                near.append(part * factor + bias)
                starts.append(start)
            near = jnp.concatenate(near, axis=0)
            peak = jnp.maximum(jnp.max(near, axis=1, keepdims=True), jnp.max(far, axis=1, keepdims=True))
            near = jnp.exp(near - peak)
            far = jnp.exp(far - peak)
            inverse = 1.0 / (jnp.sum(near, axis=1, keepdims=True) + jnp.sum(far, axis=1, keepdims=True))
            near = near.astype(jnp.bfloat16)
            mixed = lax.dot_general(far.astype(jnp.bfloat16), ctx_ref[:, vs], plain, preferred_element_type=jnp.float32)
            local = [
                lax.dot_general(
                    near[g * GRID_W : (g + 1) * GRID_W], kv_ref[pl.ds(starts[g], span), vs],
                    plain, preferred_element_type=jnp.float32)
                for g in range(group)
            ]
            mixed = (mixed + jnp.concatenate(local, axis=0)) * inverse
            attn_ref[at, ks] = mixed.astype(jnp.bfloat16)
    count = len(outs)
    own = tokens // count
    for k, out in enumerate(outs):
        block = lax.rem(me + k, count)
        out[...] = attn_ref[pl.ds(pl.multiple_of(block * own, own), own), :]
    fetch.wait()


def attend(place, query, keys, values, before, after, bias, out_weight, chunks, count):
    tokens, width = query.shape
    group = 2 if (tokens // GRID_W) % 2 == 0 else 1
    above, below = before.shape[0], after.shape[0]
    ctx_n = len(chunks) * chunks[0].shape[0]
    vmem = pl.BlockSpec(memory_space=pltpu.VMEM)
    return pl.pallas_call(
        functools.partial(attend_body, group, (above, below, len(chunks))),
        in_specs=[pl.BlockSpec(memory_space=pltpu.SMEM)] + [vmem] * 6 + [pl.BlockSpec(memory_space=pltpu.HBM)] + [vmem] * len(chunks),
        out_specs=[vmem] * (count + 1),
        out_shape=[jax.ShapeDtypeStruct((tokens // count, width), jnp.bfloat16)] * count
        + [jax.ShapeDtypeStruct(out_weight.shape, out_weight.dtype)],
        scratch_shapes=[
            pltpu.VMEM((above + tokens + below, 2 * width), jnp.bfloat16),
            pltpu.VMEM((ctx_n, 2 * width), jnp.bfloat16),
            pltpu.VMEM((tokens, width), jnp.bfloat16),
            pltpu.SemaphoreType.DMA,
        ],
        compiler_params=pltpu.CompilerParams(vmem_limit_bytes=8 * 2**20),
        name="attend",
    )(place, query, keys, values, before, after, bias, out_weight, *chunks)


def out_body(count, tp_ref, *refs):
    pieces, (w_ref, gate_ref, lat_ref, out_ref) = refs[:count], refs[count:]
    me = tp_ref[0]
    depth = pieces[0].shape[1]
    block = min(512, w_ref.shape[1])
    for n in range(0, w_ref.shape[1], block):
        cols = slice(n, n + block)
        mixed = None
        for k, piece in enumerate(pieces):
            at = lax.rem(me + (count - k), count)
            rows = w_ref[pl.ds(pl.multiple_of(at * depth, depth), depth), cols]
            part = jnp.dot(piece[...], rows, preferred_element_type=jnp.float32)
            mixed = part if mixed is None else mixed + part
        out_ref[:, cols] = (lat_ref[:, cols].astype(jnp.float32) + gate_ref[:, cols] * mixed).astype(jnp.bfloat16)


def project_out(me, pieces, out_weight, gates, residual):
    vmem = pl.BlockSpec(memory_space=pltpu.VMEM)
    return pl.pallas_call(
        functools.partial(out_body, len(pieces)),
        in_specs=[pl.BlockSpec(memory_space=pltpu.SMEM)] + [vmem] * (len(pieces) + 3),
        out_specs=vmem,
        out_shape=jax.ShapeDtypeStruct(residual.shape, jnp.bfloat16),
        compiler_params=pltpu.CompilerParams(vmem_limit_bytes=8 * 2**20),
        name="project_out",
    )(me, *pieces, out_weight, gates, residual)


def shards(
    latents, cond, ctx_cond, context, norm_gain, shift_weight, scale_weight, gate_weight,
    q_weight, k_weight, v_weight, out_weight, rel_bias,
):
    tp = lax.axis_size("tp")
    sp = lax.axis_size("sp")
    tp_at = lax.axis_index("tp")
    sp_at = lax.axis_index("sp")
    tp_rows = shift_weight.shape[0]
    after_this = lambda x, y: lax.optimization_barrier((x, y))[0]
    group = 2 if sp % 2 == 0 else 1
    near_ctx = context
    if group == 2:
        other = lax.ppermute(context, "sp", [(i, i ^ 1) for i in range(sp)])
        near_ctx = jnp.concatenate([context, other], axis=0)

    conds = jnp.stack([cond, ctx_cond])
    active = jax.nn.silu(
        lax.dynamic_slice_in_dim(conds, tp_at * tp_rows, tp_rows, 1)
    ).astype(jnp.bfloat16)
    shifts = jnp.dot(active, shift_weight, preferred_element_type=jnp.float32)
    scales = jnp.dot(active, scale_weight, preferred_element_type=jnp.float32)
    gates = jnp.dot(active[:1], gate_weight, preferred_element_type=jnp.float32)
    mod = jnp.concatenate([shifts, scales, gates], axis=0)
    mod = functools.reduce(jnp.add, [shift_by(mod, "tp", k) for k in range(1, tp)], mod)
    shifts, scales, gates = mod[0:2], mod[2:4], mod[4:5]

    h_lat = modulated_norm(latents, norm_gain, shifts[0], scales[0])
    keys = jnp.dot(h_lat, k_weight, preferred_element_type=jnp.float32).astype(jnp.bfloat16)
    values = jnp.dot(h_lat, v_weight, preferred_element_type=jnp.float32).astype(jnp.bfloat16)
    above, below = HALF * GRID_W, (WIN_ROWS - HALF - 1) * GRID_W
    up = [(i, i + 1) for i in range(sp - 1)]
    down = [(i + 1, i) for i in range(sp - 1)]
    last = jnp.concatenate([keys[-above:], values[-above:]], axis=1)
    initial = jnp.concatenate([keys[:below], values[:below]], axis=1)
    before = lax.ppermute(last, "sp", up)
    after = lax.ppermute(initial, "sp", down)

    ctx_shift, ctx_scale = after_this((shifts[1], scales[1]), (last, initial))
    h_ctx = modulated_norm(near_ctx, norm_gain, ctx_shift, ctx_scale)
    ctx_kv = jnp.concatenate(
        [jnp.dot(h_ctx, w, preferred_element_type=jnp.float32).astype(jnp.bfloat16) for w in (k_weight, v_weight)],
        axis=1,
    )
    chunks = [ctx_kv] + [shift_by(ctx_kv, "sp", k) for k in range(group, sp, group)]
    late_h = after_this(h_lat, ctx_kv)
    query = jnp.dot(late_h, q_weight, preferred_element_type=jnp.float32).astype(jnp.bfloat16)

    rows_here = latents.shape[0] // GRID_W
    place = jnp.stack([sp_at * rows_here, jnp.int32(sp * rows_here), tp_at]).astype(jnp.int32)
    *attn, late_weight = attend(
        place, query, keys, values, before, after, bias_tiles(rel_bias), out_weight, chunks, tp)
    pieces = [shift_by(part, "tp", k) if k else part for k, part in enumerate(attn)]
    own = latents.shape[0] // tp
    residual = lax.dynamic_slice_in_dim(latents, tp_at * own, own, 0)
    return project_out(tp_at.reshape(1).astype(jnp.int32), pieces, late_weight, gates, residual)


def solution(mesh):
    in_specs = (
        P("sp", None), P(), P(), P("sp", None), P(), P("tp", None), P("tp", None), P("tp", None),
        P(None, "tp"), P(None, "tp"), P(None, "tp"), P(), P("tp", None, None),
    )
    out_specs = P(("sp", "tp"), None)
    return jax.shard_map(shards, mesh=mesh, in_specs=in_specs, out_specs=out_specs, check_vma=False)
```

```python
import functools

import jax
import jax.numpy as jnp
from jax import lax
from jax.experimental import pallas as pl
from jax.experimental.pallas import tpu as pltpu
from jax.sharding import PartitionSpec as P

HEAD_DIM = 128
GRID_W = 64
WIN_ROWS = 8
WIN_COLS = 16
HALF = WIN_ROWS // 2
EPS = 1e-06
NEG_BIG = -1e30


def shift_by(x, axis, k):
    n = lax.axis_size(axis)
    return lax.ppermute(x, axis, [(i, (i + k) % n) for i in range(n)])


def ring_both_ways(own, group):
    count = lax.axis_size("sp") // group
    chunks, low, high = [own], own, own
    for step in range(1, count // 2 + 1):
        if 2 * step == count and step > 1:
            half = own.shape[0] // 2
            chunks.append(shift_by(low[:half], "sp", group))
            chunks.append(shift_by(high[half:], "sp", -group))
        elif 2 * step == count:
            chunks.append(shift_by(low, "sp", group))
        else:
            low, high = shift_by(low, "sp", group), shift_by(high, "sp", -group)
            chunks += [low, high]
    return chunks


def modulated_norm(tok_rows, gain, shift_row, scale_row):
    rows_f = tok_rows.astype(jnp.float32)
    inverse = lax.rsqrt(jnp.mean(rows_f * rows_f, axis=-1, keepdims=True) + EPS)
    return (rows_f * inverse * (gain * (1.0 + scale_row)) + shift_row).astype(jnp.bfloat16)


def bias_body(table_ref, out_ref):
    lane = lax.broadcasted_iota(jnp.int32, (GRID_W, 2 * GRID_W), 1)
    col = lane % GRID_W
    own = lax.broadcasted_iota(jnp.int32, (GRID_W, 2 * GRID_W), 0)
    first = jnp.clip(own - WIN_COLS // 2, 0, GRID_W - WIN_COLS)
    inside = (col >= first) & (col < first + WIN_COLS)
    low = lane < GRID_W
    tiles = [(h, d) for h in range(table_ref.shape[0]) for d in range(2 * WIN_ROWS - 2)]
    for h, d in tiles:
        left = jnp.broadcast_to(table_ref[h, d : d + 1, :], (GRID_W, 2 * GRID_W))
        right = jnp.broadcast_to(table_ref[h, d + 1 : d + 2, :], (GRID_W, 2 * GRID_W))
        left = pltpu.roll(left, 2 * GRID_W - (WIN_COLS - 1), 1, stride=1, stride_axis=0)
        right = pltpu.roll(right, GRID_W - (WIN_COLS - 1), 1, stride=1, stride_axis=0)
        out_ref[h, d] = jnp.where(inside, jnp.where(low, left, right), NEG_BIG)


def bias_tiles(rel_bias):
    heads = rel_bias.shape[0]
    table = jnp.pad(rel_bias, ((0, 0), (0, 1), (0, 2 * GRID_W - rel_bias.shape[2])))
    return pl.pallas_call(
        bias_body,
        in_specs=[pl.BlockSpec(memory_space=pltpu.VMEM)],
        out_specs=pl.BlockSpec(memory_space=pltpu.VMEM),
        out_shape=jax.ShapeDtypeStruct((heads, 2 * WIN_ROWS - 2, GRID_W, 2 * GRID_W), jnp.float32),
        compiler_params=pltpu.CompilerParams(vmem_limit_bytes=8 * 2**20),
        name="bias_tiles",
    )(table)


def attend_body(group, halos, place_ref, q_ref, k_ref, v_ref, up_ref, down_ref, bias_ref, w_ref, *refs):
    chunks, outs, w_out = refs[: halos[2]], refs[halos[2] : -5], refs[-5]
    kv_ref, ctx_ref, attn_ref, sem = refs[-4:]
    fetch = pltpu.make_async_copy(w_ref, w_out, sem)
    fetch.start()
    factor = HEAD_DIM ** (-0.5)
    base, total, me = place_ref[0], place_ref[1], place_ref[2]
    tokens, width = q_ref.shape
    above, below = halos[0], halos[1]
    kv_ref[0:above, :] = up_ref[...]
    kv_ref[above : above + tokens, 0:width] = k_ref[...]
    kv_ref[above : above + tokens, width:] = v_ref[...]
    kv_ref[above + tokens : above + tokens + below, :] = down_ref[...]
    filled = 0
    for chunk in chunks:
        ctx_ref[filled : filled + chunk.shape[0], :] = chunk[...]
        filled += chunk.shape[0]
    contract_last = (((1,), (1,)), ((), ()))
    plain = (((1,), (0,)), ((), ()))
    span = WIN_ROWS * GRID_W
    for h in range(width // HEAD_DIM):
        ks = slice(h * HEAD_DIM, (h + 1) * HEAD_DIM)
        vs = slice(width + h * HEAD_DIM, width + (h + 1) * HEAD_DIM)
        for r0 in range(0, tokens // GRID_W, group):
            at = slice(r0 * GRID_W, (r0 + group) * GRID_W)
            q = q_ref[at, ks]
            far = lax.dot_general(q, ctx_ref[:, ks], contract_last, preferred_element_type=jnp.float32) * factor
            near, starts = [], []
            for g in range(group):
                row = base + r0 + g
                first = jnp.clip(row - HALF, 0, total - WIN_ROWS)
                start = pl.multiple_of((first - base + HALF) * GRID_W, GRID_W)
                delta = first - row + WIN_ROWS - 1
                keys = kv_ref[pl.ds(start, span), ks]
                part = lax.dot_general(q[g * GRID_W : (g + 1) * GRID_W], keys, contract_last, preferred_element_type=jnp.float32)
                bias = jnp.concatenate([bias_ref[h, delta + 2 * t] for t in range(WIN_ROWS // 2)], axis=1)
                near.append(part * factor + bias)
                starts.append(start)
            near = jnp.concatenate(near, axis=0)
            peak = jnp.maximum(jnp.max(near, axis=1, keepdims=True), jnp.max(far, axis=1, keepdims=True))
            near = jnp.exp(near - peak)
            far = jnp.exp(far - peak)
            inverse = 1.0 / (jnp.sum(near, axis=1, keepdims=True) + jnp.sum(far, axis=1, keepdims=True))
            near = near.astype(jnp.bfloat16)
            mixed = lax.dot_general(far.astype(jnp.bfloat16), ctx_ref[:, vs], plain, preferred_element_type=jnp.float32)
            local = [
                lax.dot_general(
                    near[g * GRID_W : (g + 1) * GRID_W], kv_ref[pl.ds(starts[g], span), vs],
                    plain, preferred_element_type=jnp.float32)
                for g in range(group)
            ]
            mixed = (mixed + jnp.concatenate(local, axis=0)) * inverse
            attn_ref[at, ks] = mixed.astype(jnp.bfloat16)
    count = len(outs)
    own = tokens // count
    for k, out in enumerate(outs):
        block = lax.rem(me + k, count)
        out[...] = attn_ref[pl.ds(pl.multiple_of(block * own, own), own), :]
    fetch.wait()


def attend(place, query, keys, values, before, after, bias, out_weight, chunks, count):
    tokens, width = query.shape
    group = 2 if (tokens // GRID_W) % 2 == 0 else 1
    above, below = before.shape[0], after.shape[0]
    ctx_n = sum(chunk.shape[0] for chunk in chunks)
    vmem = pl.BlockSpec(memory_space=pltpu.VMEM)
    return pl.pallas_call(
        functools.partial(attend_body, group, (above, below, len(chunks))),
        in_specs=[pl.BlockSpec(memory_space=pltpu.SMEM)] + [vmem] * 6 + [pl.BlockSpec(memory_space=pltpu.HBM)] + [vmem] * len(chunks),
        out_specs=[vmem] * (count + 1),
        out_shape=[jax.ShapeDtypeStruct((tokens // count, width), jnp.bfloat16)] * count
        + [jax.ShapeDtypeStruct(out_weight.shape, out_weight.dtype)],
        scratch_shapes=[
            pltpu.VMEM((above + tokens + below, 2 * width), jnp.bfloat16),
            pltpu.VMEM((ctx_n, 2 * width), jnp.bfloat16),
            pltpu.VMEM((tokens, width), jnp.bfloat16),
            pltpu.SemaphoreType.DMA,
        ],
        compiler_params=pltpu.CompilerParams(vmem_limit_bytes=8 * 2**20),
        name="attend",
    )(place, query, keys, values, before, after, bias, out_weight, *chunks)


def out_body(count, tp_ref, *refs):
    pieces, (w_ref, gate_ref, lat_ref, out_ref) = refs[:count], refs[count:]
    me = tp_ref[0]
    depth = pieces[0].shape[1]
    block = min(512, w_ref.shape[1])
    for n in range(0, w_ref.shape[1], block):
        cols = slice(n, n + block)
        mixed = None
        for k, piece in enumerate(pieces):
            at = lax.rem(me + (count - k), count)
            rows = w_ref[pl.ds(pl.multiple_of(at * depth, depth), depth), cols]
            part = jnp.dot(piece[...], rows, preferred_element_type=jnp.float32)
            mixed = part if mixed is None else mixed + part
        out_ref[:, cols] = (lat_ref[:, cols].astype(jnp.float32) + gate_ref[:, cols] * mixed).astype(jnp.bfloat16)


def project_out(me, pieces, out_weight, gates, residual):
    vmem = pl.BlockSpec(memory_space=pltpu.VMEM)
    return pl.pallas_call(
        functools.partial(out_body, len(pieces)),
        in_specs=[pl.BlockSpec(memory_space=pltpu.SMEM)] + [vmem] * (len(pieces) + 3),
        out_specs=vmem,
        out_shape=jax.ShapeDtypeStruct(residual.shape, jnp.bfloat16),
        compiler_params=pltpu.CompilerParams(vmem_limit_bytes=8 * 2**20),
        name="project_out",
    )(me, *pieces, out_weight, gates, residual)


def shards(
    latents, cond, ctx_cond, context, norm_gain, shift_weight, scale_weight, gate_weight,
    q_weight, k_weight, v_weight, out_weight, rel_bias,
):
    tp = lax.axis_size("tp")
    sp = lax.axis_size("sp")
    tp_at = lax.axis_index("tp")
    sp_at = lax.axis_index("sp")
    tp_rows = shift_weight.shape[0]
    after_this = lambda x, y: lax.optimization_barrier((x, y))[0]
    group = 2 if sp % 2 == 0 else 1
    near_ctx = context
    if group == 2:
        other = lax.ppermute(context, "sp", [(i, i ^ 1) for i in range(sp)])
        near_ctx = jnp.concatenate([context, other], axis=0)

    conds = jnp.stack([cond, ctx_cond])
    active = jax.nn.silu(
        lax.dynamic_slice_in_dim(conds, tp_at * tp_rows, tp_rows, 1)
    ).astype(jnp.bfloat16)
    shifts = jnp.dot(active, shift_weight, preferred_element_type=jnp.float32)
    scales = jnp.dot(active, scale_weight, preferred_element_type=jnp.float32)
    gates = jnp.dot(active[:1], gate_weight, preferred_element_type=jnp.float32)
    mod = jnp.concatenate([shifts, scales, gates], axis=0)
    mod = functools.reduce(jnp.add, [shift_by(mod, "tp", k) for k in range(1, tp)], mod)
    shifts, scales, gates = mod[0:2], mod[2:4], mod[4:5]

    h_lat = modulated_norm(latents, norm_gain, shifts[0], scales[0])
    keys = jnp.dot(h_lat, k_weight, preferred_element_type=jnp.float32).astype(jnp.bfloat16)
    values = jnp.dot(h_lat, v_weight, preferred_element_type=jnp.float32).astype(jnp.bfloat16)
    above, below = HALF * GRID_W, (WIN_ROWS - HALF - 1) * GRID_W
    up = [(i, i + 1) for i in range(sp - 1)]
    down = [(i + 1, i) for i in range(sp - 1)]
    last = jnp.concatenate([keys[-above:], values[-above:]], axis=1)
    initial = jnp.concatenate([keys[:below], values[:below]], axis=1)
    before = lax.ppermute(last, "sp", up)
    after = lax.ppermute(initial, "sp", down)

    ctx_shift, ctx_scale = after_this((shifts[1], scales[1]), (last, initial))
    h_ctx = modulated_norm(near_ctx, norm_gain, ctx_shift, ctx_scale)
    ctx_kv = jnp.concatenate(
        [jnp.dot(h_ctx, w, preferred_element_type=jnp.float32).astype(jnp.bfloat16) for w in (k_weight, v_weight)],
        axis=1,
    )
    chunks = ring_both_ways(ctx_kv, group)
    late_h = after_this(h_lat, ctx_kv)
    query = jnp.dot(late_h, q_weight, preferred_element_type=jnp.float32).astype(jnp.bfloat16)

    rows_here = latents.shape[0] // GRID_W
    place = jnp.stack([sp_at * rows_here, jnp.int32(sp * rows_here), tp_at]).astype(jnp.int32)
    *attn, late_weight = attend(
        place, query, keys, values, before, after, bias_tiles(rel_bias), out_weight, chunks, tp)
    pieces = [shift_by(part, "tp", k) if k else part for k, part in enumerate(attn)]
    own = latents.shape[0] // tp
    residual = lax.dynamic_slice_in_dim(latents, tp_at * own, own, 0)
    return project_out(tp_at.reshape(1).astype(jnp.int32), pieces, late_weight, gates, residual)


def solution(mesh):
    in_specs = (
        P("sp", None), P(), P(), P("sp", None), P(), P("tp", None), P("tp", None), P("tp", None),
        P(None, "tp"), P(None, "tp"), P(None, "tp"), P(), P("tp", None, None),
    )
    out_specs = P(("sp", "tp"), None)
    return jax.shard_map(shards, mesh=mesh, in_specs=in_specs, out_specs=out_specs, check_vma=False)
```
